32 devices in a mesh: gr: 2 (over core), sp: 8 (over z, y), tp: 2 (over x).
Axes of the slice: x: 2, y: 2, z: 4, core: 2. Of those that a mesh axis runs over, the one named last changes fastest.
Arguments:
- tokens: bfloat16 [4, 2048, 2048], P('gr', ('sp', 'tp')), parts along dimension 0, may hold values from -6 to 6
- key_weight: bfloat16 [2048, 1024], P('sp'), may hold values from -0.125 to 0.125
- value_weight: bfloat16 [2048, 1024], P('sp'), may hold values from -0.125 to 0.125
- queries: bfloat16 [4, 1024], P('gr'), parts along dimension 0, may hold values from -6 to 6
- head_offset: float32 [16], replicated, may hold values from -14 to -3.5
- key_bias: bfloat16 [4, 2048, 16], P('gr', ('sp', 'tp')), parts along dimension 0, may hold values from -0.5 to 12.9
Outputs:
- key_cache: bfloat16 [4, 2048, 1024], P('gr', 'sp', 'tp'), parts along dimension 0
- value_cache: bfloat16 [4, 2048, 1024], P('gr', 'sp', 'tp'), parts along dimension 0
- bias_cache: bfloat16 [4, 2048, 16], P('gr', 'sp', 'tp'), parts along dimension 0
- reading: float32 [4, 1024], P('gr', 'tp'), parts along dimension 0
The draws below stay inside these ranges and needn't reach their ends.
There are 2 independent parts, one for each index of `gr`. The reference program is written for one: setup_inputs(seed, part) draws one part's arguments, and reference() takes and returns one part's arrays. A program takes and returns all parts, laid end to end along the dimension named above; an argument that names none is the same for every part. Nothing has to cross between parts.
All inputs are finite; a program needn't handle non-finite values.
Results may differ from the reference program's by a relative error of at most 0.0052.
Values may be sent and summed in bfloat16 or wider, within the bound.
No kernel may reach another device: no remote copies, remote signals or barrier semaphores. Data moves between devices by JAX's collectives and lax.ppermute only.
A program may use at most 64 MiB of HBM per device.

```python
import jax
import jax.numpy as jnp
from jax import lax

D = 2048
HEADS = 16
HEAD_DIM = 64
GROUP_SEQUENCES = 2
POS_DEV = 128
PROMPT_LENGTH = 2048


def draw_head_offset(key, part):
    key_a, key_b, key_c, order_key = jax.random.split(jax.random.fold_in(key, 11), 4)
    scale_base = jnp.log(jnp.float32(PROMPT_LENGTH) * 14.6)
    slow_rate = jnp.log(jax.random.uniform(key_a, (HEADS,), jnp.float32, 1.0, 2.3)) - scale_base
    middle_rate = jnp.log(jax.random.uniform(key_c, (HEADS,), jnp.float32, 5.0, 9.0)) - scale_base
    fast_rate = jax.random.uniform(key_b, (HEADS,), jnp.float32, -5.0, -3.5)
    ranks = jax.random.permutation(order_key, HEADS)
    chosen = jnp.where(ranks < HEADS // 2, slow_rate, jnp.where(ranks < 3 * HEADS // 4, middle_rate, fast_rate))
    return chosen.astype(jnp.float32)


def draw_key_bias(key, part):
    key_a, key_b, third_random_key, fourth_random_key = jax.random.split(jax.random.fold_in(key, 23), 4)
    block_count = PROMPT_LENGTH // POS_DEV
    block_tier = jax.random.uniform(key_a, (GROUP_SEQUENCES, block_count, 1, HEADS), jnp.float32, 0.0, 3.4)
    block_tier = jnp.broadcast_to(block_tier, (GROUP_SEQUENCES, block_count, POS_DEV, HEADS)).reshape(GROUP_SEQUENCES, PROMPT_LENGTH, HEADS)
    coarse_portion = jnp.clip(0.25 * jax.random.normal(key_b, (GROUP_SEQUENCES, PROMPT_LENGTH, HEADS), jnp.float32), -0.5, 0.5)
    spike_places = jax.random.randint(third_random_key, (GROUP_SEQUENCES, 3), 0, PROMPT_LENGTH)
    spike_mask = jnp.any(jnp.arange(PROMPT_LENGTH)[None, :, None] == spike_places[:, None, :], axis=-1)
    spike_length = jax.random.uniform(fourth_random_key, (GROUP_SEQUENCES, PROMPT_LENGTH, 1), jnp.float32, 7.5, 9.0)
    grand_sum = block_tier + coarse_portion + jnp.where(spike_mask[:, :, None], spike_length, 0.0)
    return grand_sum.astype(jnp.bfloat16)


def levels(stream_key, shape, shards, smallest, high):
    factor_of = 1.0
    for dim, parts in shards:
        heights = jax.random.uniform(jax.random.fold_in(jax.random.fold_in(stream_key, 6), dim), (parts,), jnp.float32, smallest / len(shards), high / len(shards))
        factor_of = factor_of * jnp.repeat(jnp.exp(heights), shape[dim] // parts).reshape((-1,) + (1,) * (len(shape) - 1 - dim))
    return factor_of


def scatter_about(own_key, dims, scale, reach, pieces=(), kind=jnp.bfloat16):
    result = jax.random.normal(own_key, dims, jnp.float32) * scale
    if len(pieces) > 0:
        result = levels(own_key, dims, pieces, -0.22, 0.18) * result
    return jnp.clip(result, min=-reach, max=reach).astype(kind)


def setup_inputs(seed: int = 0, part: int = 0) -> dict:
    arg_keys = jax.random.split(jax.random.key(seed), 7)
    part_splits = jax.random.split(jax.random.fold_in(arg_keys[6], part), 7)
    return {
        "tokens": scatter_about(part_splits[0], (GROUP_SEQUENCES, PROMPT_LENGTH, D), 1.0, 6.0, ((1, 16),)),
        "key_weight": scatter_about(arg_keys[1], (D, HEADS * HEAD_DIM), D ** -0.5, 0.125, ((0, 8),)),
        "value_weight": scatter_about(arg_keys[2], (D, HEADS * HEAD_DIM), D ** -0.5, 0.125, ((0, 8),)),
        "queries": scatter_about(part_splits[3], (GROUP_SEQUENCES, HEADS * HEAD_DIM), 1.0, 6.0),
        "head_offset": draw_head_offset(jax.random.fold_in(arg_keys[6], 71), part),
        "key_bias": draw_key_bias(jax.random.fold_in(jax.random.fold_in(arg_keys[6], part), 71), part),
    }


def reference(tokens, key_weight, value_weight, queries, head_offset, key_bias):
    score_scale = HEAD_DIM ** (-0.5)

    def one_sequence(inputs):
        tok_rows, key_offsets, query_row = inputs
        key_rows = jnp.dot(tok_rows, key_weight, preferred_element_type=jnp.float32).astype(jnp.bfloat16)
        value_rows = jnp.dot(tok_rows, value_weight, preferred_element_type=jnp.float32).astype(jnp.bfloat16)
        key_heads = key_rows.reshape(PROMPT_LENGTH, HEADS, HEAD_DIM).astype(jnp.float32)
        value_heads = value_rows.reshape(PROMPT_LENGTH, HEADS, HEAD_DIM).astype(jnp.float32)
        query_heads = query_row.reshape(HEADS, HEAD_DIM).astype(jnp.float32)
        logits = jnp.einsum('thc,hc->ht', key_heads, query_heads) * score_scale
        logits = logits + head_offset[:, None] + key_offsets.astype(jnp.float32).T
        fading = jax.nn.log_sigmoid(-logits)
        beyond = lax.cumsum(fading, axis=1, reverse=True) - fading
        weights = jnp.exp(jax.nn.log_sigmoid(logits) + beyond).astype(jnp.bfloat16)
        mixture = jnp.einsum('ht,thc->hc', weights.astype(jnp.float32), value_heads)
        normed = mixture * lax.rsqrt(lax.optimization_barrier(jnp.mean(mixture * mixture, axis=1, keepdims=True)) + 1e-06)
        return (key_rows, value_rows, normed.reshape(HEADS * HEAD_DIM))
    key_rows, value_rows, reading = lax.map(one_sequence, (tokens, key_bias, queries))
    return (key_rows, value_rows, key_bias, reading)
```

```python
import functools

import jax
import jax.numpy as jnp
from jax import lax
from jax.experimental import pallas as pl
from jax.experimental.pallas import tpu as pltpu
from jax.sharding import PartitionSpec as P


BF16 = jnp.bfloat16
F32 = jnp.float32


def ring_at(place, count):
    half = (count + 1) // 2
    return jnp.where(place < half, 2 * place, 2 * (count - 1 - place) + 1)


def place_of(index, count):
    return jnp.where(index % 2 == 0, index // 2, count - 1 - (index - 1) // 2)


def ring_perm(count):
    order = list(range(0, count, 2)) + list(range(1, count, 2))[::-1]
    pairs = []
    for p in range(count):
        here, there = order[p], order[(p + 1) % count]
        pairs.append((here, there))
        pairs.append((count + there, count + here))
    return pairs


def attend(
    sizes, order, query, offset, bias, *refs
):
    tp_count, sp_count, seqs, pos, depth, cols, heads, head_dim = sizes
    toks = refs[:tp_count]
    refs = refs[tp_count:]
    k_parts, v_parts = refs[:sp_count], refs[sp_count : 2 * sp_count]
    key_out, value_out, stat_out = refs[2 * sp_count : 2 * sp_count + 3]
    x, wk, wv, acc, keys, values, sem_x, sem_k, sem_v, sem_o = refs[2 * sp_count + 3 :]
    rows = seqs * pos
    span = tp_count * pos
    group = lax.axis_index("gr")
    me_tp = lax.axis_index("tp")

    def copy_w(source, target, slot, sem):
        rows_at = pl.ds(pl.multiple_of(order[slot] * depth, depth), depth)
        return pltpu.make_async_copy(source, target.at[rows_at], sem.at[slot])

    def project(at, size, first):
        for t in range(tp_count):
            part = x[t, :, pl.ds(at, size)]
            for n, w in enumerate((wk, wv)):
                product = jnp.dot(part, w[pl.ds(at, size)], preferred_element_type=F32)
                if first:
                    acc[t, n] = product
                else:
                    acc[t, n] += product

    for t in range(tp_count):
        pltpu.make_async_copy(toks[t], x.at[t], sem_x.at[t]).start()
    last = sp_count - 1
    for j in range(last):
        copy_w(k_parts[j], wk, j, sem_k).start()
        copy_w(v_parts[j], wv, j, sem_v).start()

    @pl.when(group == 0)
    def _():
        copy_w(k_parts[last], wk, last, sem_k).start()
        copy_w(v_parts[last], wv, last, sem_v).start()

    @pl.when(group != 0)
    def _():
        copy_w(v_parts[last], wk, last, sem_k).start()
        copy_w(k_parts[last], wv, last, sem_v).start()

    for t in range(tp_count):
        pltpu.make_async_copy(toks[t], x.at[t], sem_x.at[t]).wait()
    aligned = depth % 128 == 0
    for j in range(sp_count):
        copy_w(k_parts[j], wk, j, sem_k).wait()
        copy_w(v_parts[j], wv, j, sem_v).wait()
        if aligned:
            project(pl.multiple_of(order[j] * depth, depth), depth, j == 0)
    if not aligned:
        width = sp_count * depth
        block = 256 if width % 256 == 0 else width
        for at in range(0, width, block):
            project(at, block, at == 0)
    for t in range(tp_count):
        start = pl.multiple_of(lax.rem(me_tp + t, tp_count) * pos, pos)
        for s in range(seqs):
            piece = slice(s * pos, (s + 1) * pos)
            keys[s, pl.ds(start, pos), :] = acc[t, 0, piece].astype(BF16)
            values[s, pl.ds(start, pos), :] = acc[t, 1, piece].astype(BF16)
    out_k = pltpu.make_async_copy(keys, key_out, sem_o.at[0])
    out_v = pltpu.make_async_copy(values, value_out, sem_o.at[1])
    out_k.start()
    out_v.start()
    scale = head_dim**-0.5
    lane_head = lax.broadcasted_iota(jnp.int32, (heads, cols), 1) // head_dim
    own_head = lane_head == lax.broadcasted_iota(jnp.int32, (heads, cols), 0)
    above = lax.broadcasted_iota(jnp.int32, (span, span), 0) > lax.broadcasted_iota(
        jnp.int32, (span, span), 1
    )
    later = jnp.where(above, 1.0, 0.0).astype(F32)
    for s in range(seqs):
        q = jnp.where(own_head, jnp.broadcast_to(query[s : s + 1], (heads, cols)), 0).astype(BF16)
        logits = lax.dot_general(
            q, keys[s], (((1,), (1,)), ((), ())), preferred_element_type=F32
        )
        logits = logits * scale + offset[...] + bias[s]
        soft = jnp.log1p(jnp.exp(-jnp.abs(logits)))
        fading = -jnp.maximum(logits, 0.0) - soft
        rising = jnp.minimum(logits, 0.0) - soft
        within = jnp.dot(
            fading, later, preferred_element_type=F32, precision=lax.Precision.HIGHEST
        )
        total = within[:, :1] + fading[:, :1]
        weights = jnp.exp(rising + within)
        high = weights.astype(BF16)
        low = (weights - high.astype(F32)).astype(BF16)
        spread = jnp.dot(high, values[s], preferred_element_type=F32)
        spread += jnp.dot(low, values[s], preferred_element_type=F32)
        spread = jnp.where(own_head, spread, 0.0)
        mixture = spread[:, :head_dim]
        for h in range(1, heads):
            mixture += spread[:, h * head_dim : (h + 1) * head_dim]
        stat_out[s] = jnp.concatenate(
            [mixture, jnp.broadcast_to(total, (heads, 128 - head_dim))], axis=1
        )
    out_k.wait()
    out_v.wait()


def per_device(tokens, key_weight, value_weight, queries, head_offset, key_bias):
    seqs, pos, width = tokens.shape
    depth, kv_width = key_weight.shape
    all_heads = head_offset.shape[0]
    head_dim = kv_width // all_heads
    tp_count, sp_count = lax.axis_size("tp"), lax.axis_size("sp")
    tp, sp, gr = lax.axis_index("tp"), lax.axis_index("sp"), lax.axis_index("gr")
    cols = kv_width // tp_count
    heads = all_heads // tp_count
    span = tp_count * pos

    def shift(array, step):
        return lax.ppermute(array, "tp", [((i + step) % tp_count, i) for i in range(tp_count)])

    rows = tokens.reshape(seqs * pos, width)
    toks = [rows] + [shift(rows, t) for t in range(1, tp_count)]
    biases = []
    for t in range(tp_count):
        target = lax.rem(tp - t + tp_count, tp_count)
        part = lax.dynamic_slice_in_dim(key_bias, target * heads, heads, 2)
        biases.append(part if t == 0 else shift(part, t))
    bias_cache = jnp.concatenate(biases, axis=1)
    if tp_count > 1:
        bias_cache = jnp.roll(bias_cache, tp * pos, axis=1)

    col = tp * cols
    key_part = lax.dynamic_slice_in_dim(key_weight, col, cols, 1)
    value_part = lax.dynamic_slice_in_dim(value_weight, col, cols, 1)
    perm = ring_perm(sp_count)

    def onward(array):
        return lax.ppermute(array, ("gr", "sp"), perm)

    def across(array):
        return lax.ppermute(array, "gr", [(0, 1), (1, 0)])

    k_parts, v_parts = [key_part], [value_part]
    k_now, v_now = key_part, value_part
    for _ in range(sp_count // 2 - 1):
        k_now, v_now = onward(k_now), onward(v_now)
        k_parts += [k_now, across(k_now)]
        v_parts += [v_now, across(v_now)]
    far = onward(jnp.where(gr == 0, k_now, v_now))
    k_parts.append(far)
    v_parts.append(across(far))
    turn = jnp.where(gr == 0, -1, 1)
    place = place_of(sp, sp_count)
    steps = [0]
    for j in range(1, sp_count // 2):
        steps += [j, -j]
    steps.append(sp_count // 2)
    places = lax.rem(place + turn * jnp.array(steps, jnp.int32) + sp_count, sp_count)
    order = ring_at(places, sp_count).astype(jnp.int32)

    query = lax.dynamic_slice_in_dim(queries, col, cols, 1)
    offset = lax.dynamic_slice_in_dim(head_offset, tp * heads, heads, 0)[:, None]
    bias_rows = jnp.transpose(bias_cache.astype(F32), (0, 2, 1))

    sizes = (tp_count, sp_count, seqs, pos, depth, cols, heads, head_dim)
    vmem = pl.BlockSpec(memory_space=pltpu.VMEM)
    hbm = pl.BlockSpec(memory_space=pl.ANY)
    key_cache, value_cache, stat = pl.pallas_call(
        functools.partial(attend, sizes),
        out_shape=(
            jax.ShapeDtypeStruct((seqs, span, cols), BF16),
            jax.ShapeDtypeStruct((seqs, span, cols), BF16),
            jax.ShapeDtypeStruct((seqs, heads, 128), F32),
        ),
        in_specs=[pl.BlockSpec(memory_space=pltpu.SMEM), vmem, vmem, vmem]
        + [hbm] * (tp_count + 2 * sp_count),
        out_specs=(hbm, hbm, vmem),
        scratch_shapes=[
            pltpu.VMEM((tp_count, seqs * pos, width), BF16),
            pltpu.VMEM((width, cols), BF16),
            pltpu.VMEM((width, cols), BF16),
            pltpu.VMEM((tp_count, 2, seqs * pos, cols), F32),
            pltpu.VMEM((seqs, span, cols), BF16),
            pltpu.VMEM((seqs, span, cols), BF16),
            pltpu.SemaphoreType.DMA((tp_count,)),
            pltpu.SemaphoreType.DMA((sp_count,)),
            pltpu.SemaphoreType.DMA((sp_count,)),
            pltpu.SemaphoreType.DMA((2,)),
        ],
        name="attend",
    )(order, query, offset, bias_rows, *toks, *k_parts, *v_parts)

    reach = 1
    while reach < sp_count:
        other = lax.ppermute(stat, "sp", [(i, i ^ reach) for i in range(sp_count)])
        first = (sp // reach) % 2 == 0
        early = jnp.where(first, stat, other)
        late = jnp.where(first, other, stat)
        fade = late[..., head_dim:]
        mixture = early[..., :head_dim] * jnp.exp(fade[..., :1]) + late[..., :head_dim]
        stat = jnp.concatenate([mixture, early[..., head_dim:] + fade], axis=-1)
        reach *= 2
    mixture = stat[..., :head_dim]
    norm = lax.rsqrt(jnp.mean(mixture * mixture, axis=-1, keepdims=True) + 1e-06)
    reading = (mixture * norm).reshape(seqs, cols)
    return key_cache, value_cache, bias_cache, reading


def solution(mesh):
    in_specs = (
        P("gr", ("sp", "tp"), None),
        P("sp", None),
        P("sp", None),
        P("gr", None),
        P(),
        P("gr", ("sp", "tp"), None),
    )
    out_specs = (P("gr", "sp", "tp"), P("gr", "sp", "tp"), P("gr", "sp", "tp"), P("gr", "tp"))
    return jax.shard_map(
        per_device, mesh=mesh, in_specs=in_specs, out_specs=out_specs, check_vma=False
    )
```

```python
import functools

import jax
import jax.numpy as jnp
from jax import lax
from jax.experimental import pallas as pl
from jax.experimental.pallas import tpu as pltpu
from jax.sharding import PartitionSpec as P


BF16 = jnp.bfloat16
F32 = jnp.float32


def wrapped(value, count):
    value = jnp.where(value < 0, value + count, value)
    return jnp.where(value >= count, value - count, value)


def ring_perm(count):
    order = list(range(0, count, 2)) + list(range(1, count, 2))[::-1]
    pairs = []
    for p in range(count):
        here, there = order[p], order[(p + 1) % count]
        pairs.append((here, there))
        pairs.append((count + there, count + here))
    return pairs


def origins(slots, count):
    index, forward = lax.axis_index("sp"), lax.axis_index("gr") == 0
    half = lax.shift_right_logical(index, 1)
    place = jnp.where(lax.bitwise_and(index, 1) == 0, half, count - 1 - half)
    found = []
    for slot in slots:
        away = (slot + 1) // 2 * (-1 if slot % 2 == 1 else 1)
        at = wrapped(place + jnp.where(forward, away, -away), count)
        found.append(jnp.where(at < count // 2, 2 * at, 2 * (count - 1 - at) + 1))
    return found


def taken(slots, count, depth, x):
    if count == 1:
        return x[...]
    parts = []
    for at in origins(slots, count):
        at = pl.multiple_of(at * depth, depth)
        parts.append(x[:, pl.ds(at, depth)])
    return parts[0] if len(parts) == 1 else jnp.concatenate(parts, axis=1)


def stacked(refs):
    parts = [ref[...] for ref in refs]
    return parts[0] if len(parts) == 1 else jnp.concatenate(parts, axis=0)


def dot(x, w):
    return jnp.dot(x, w, preferred_element_type=F32)


def early_kernel(count, total, depth, x, *refs):
    part = taken(range(count), total, depth, x)
    for i in range(2):
        refs[2 * count][i] = dot(part, stacked(refs[i * count : (i + 1) * count]))


def middle_kernel(tp_count, early, count, total, depth, before, *refs):
    toks, refs = refs[:tp_count], refs[tp_count:]
    weights, acc = (refs[:count], refs[count : 2 * count]), refs[2 * count]
    rows = before.shape[1]
    for t in range(tp_count):
        start = early if t == 0 else 0
        part = taken(range(start, count), total, depth, toks[t])
        for i in range(2):
            product = dot(part, stacked(weights[i][start:]))
            if t == 0:
                product += before[i]
            acc[i, t * rows : (t + 1) * rows] = product


def attend_kernel(sizes, query, offset, *refs):
    tp_count, early, slots, count, seqs, pos, depth, cols, heads, head_dim = sizes
    acc, refs = (refs[0], refs[1:]) if early else (None, refs)
    toks, refs = refs[:tp_count], refs[tp_count:]
    first, second = refs[: len(slots)], refs[len(slots) : 2 * len(slots)]
    biases, (keys, values, bias_out, stat_out, bias) = (
        refs[2 * len(slots) : -5],
        refs[-5:],
    )
    span = tp_count * pos
    rows = seqs * pos
    swapped = lax.axis_index("gr") != 0
    me_tp = lax.axis_index("tp")
    for t in range(tp_count):
        part = taken(slots, count, depth, toks[t])
        one, two = dot(part, stacked(first)), dot(part, stacked(second))
        if early:
            one += acc[0, t * rows : (t + 1) * rows]
            two += acc[1, t * rows : (t + 1) * rows]
        start = pl.multiple_of(wrapped(me_tp + t, tp_count) * pos, pos)
        for s in range(seqs):
            piece = slice(s * pos, (s + 1) * pos)
            keys[s, pl.ds(start, pos), :] = jnp.where(swapped, two[piece], one[piece]).astype(BF16)
            values[s, pl.ds(start, pos), :] = jnp.where(swapped, one[piece], two[piece]).astype(BF16)
        for s in range(seqs):
            part = biases[t][s].astype(F32)
            bias[s * heads : (s + 1) * heads, pl.ds(start, pos)] = part + offset[...]
            bias_out[s, :, pl.ds(start, pos)] = biases[t][s]
    lane_head = lax.broadcasted_iota(jnp.int32, (heads, cols), 1) // head_dim
    own_head = lane_head == lax.broadcasted_iota(jnp.int32, (heads, cols), 0)
    logits = []
    for s in range(seqs):
        q = jnp.where(own_head, jnp.broadcast_to(query[s : s + 1], (heads, cols)), 0).astype(BF16)
        logits.append(
            lax.dot_general(q, keys[s], (((1,), (1,)), ((), ())), preferred_element_type=F32)
        )
    logits = jnp.concatenate(logits, axis=0) * (head_dim**-0.5) + bias[...]
    soft = jnp.log1p(jnp.exp(-jnp.abs(logits)))
    fading = -jnp.maximum(logits, 0.0) - soft
    rising = jnp.minimum(logits, 0.0) - soft
    above = lax.broadcasted_iota(jnp.int32, (span, span), 0) > lax.broadcasted_iota(
        jnp.int32, (span, span), 1
    )
    within = jnp.dot(
        fading,
        jnp.where(above, 1.0, 0.0).astype(F32),
        preferred_element_type=F32,
        precision=lax.Precision.HIGHEST,
    )
    total = within[:, :1] + fading[:, :1]
    weights = jnp.exp(rising + within)
    high = weights.astype(BF16)
    low = (weights - high.astype(F32)).astype(BF16)
    for s in range(seqs):
        mine = slice(s * heads, (s + 1) * heads)
        spread = dot(jnp.concatenate([high[mine], low[mine]], axis=0), values[s])
        spread = spread[:heads] + spread[heads:]
        stat_out[0, s : s + 1] = jnp.sum(jnp.where(own_head, spread, 0.0), axis=0, keepdims=True)
        totals = jnp.where(own_head, jnp.broadcast_to(total[mine], (heads, cols)), 0.0)
        stat_out[1, s : s + 1] = jnp.sum(totals, axis=0, keepdims=True)


def first_kernel(cols, keys, values, first, sem):
    at = pl.ds(pl.multiple_of(lax.axis_index("tp") * cols, cols), cols)
    source = [pltpu.make_async_copy(w.at[:, at], first, sem) for w in (keys, values)]
    forward = lax.axis_index("gr") == 0
    pl.when(forward)(source[0].start)
    pl.when(jnp.logical_not(forward))(source[1].start)
    source[0].wait()


def second_kernel(sizes, keys, values, tokens, queries, offsets, biases, *refs):
    tp_count, heads, cols = sizes
    second, rows, query, offset = refs[:4]
    parts, (offsets_here, biases_here, sems) = refs[4:-3], refs[-3:]
    me = lax.axis_index("tp")
    at = pl.ds(pl.multiple_of(me * cols, cols), cols)
    source = [pltpu.make_async_copy(w.at[:, at], second, sems.at[0]) for w in (values, keys)]
    forward = lax.axis_index("gr") == 0
    pl.when(forward)(source[0].start)
    pl.when(jnp.logical_not(forward))(source[1].start)
    copies = [
        pltpu.make_async_copy(biases, biases_here, sems.at[1]),
        pltpu.make_async_copy(offsets, offsets_here, sems.at[2]),
        pltpu.make_async_copy(queries.at[:, at], query, sems.at[3]),
        pltpu.make_async_copy(tokens, rows, sems.at[4]),
    ]
    for copy in copies:
        copy.start()
    copies[0].wait()
    copies[1].wait()
    shape = (heads, offsets.shape[1])
    wanted = lax.broadcasted_iota(jnp.int32, shape, 0) + me * heads
    found = lax.broadcasted_iota(jnp.int32, shape, 1) == wanted
    picked = jnp.where(found, jnp.broadcast_to(offsets_here[...], shape), 0.0)
    offset[...] = jnp.broadcast_to(jnp.sum(picked, axis=1, keepdims=True), offset.shape)
    every = biases_here[...].astype(F32)
    for t, part in enumerate(parts):
        target = wrapped(me - t, tp_count)
        chosen = every[:, :heads]
        for n in range(1, tp_count):
            chosen = jnp.where(target == n, every[:, n * heads : (n + 1) * heads], chosen)
        part[...] = chosen.astype(BF16)
    source[0].wait()
    copies[2].wait()
    copies[3].wait()


def store_kernel(keys, values, bias, key_out, value_out, bias_out, sems):
    pairs = ((keys, key_out), (values, value_out), (bias, bias_out))
    copies = [pltpu.make_async_copy(a, b, sems.at[i]) for i, (a, b) in enumerate(pairs)]
    for copy in copies:
        copy.start()
    for copy in copies:
        copy.wait()


def combine_kernel(reach, head_dim, last, mine, other, out):
    first = lax.bitwise_and(lax.axis_index("sp"), reach) == 0
    mine_mix, mine_total = mine[0], mine[1]
    other_mix, other_total = other[0], other[1]
    early = jnp.where(first, mine_mix, other_mix)
    late = jnp.where(first, other_mix, mine_mix)
    fade = jnp.where(first, other_total, mine_total)
    mixture = early * jnp.exp(fade) + late
    if not last:
        out[0] = mixture
        out[1] = mine_total + other_total
        return
    square = mixture * mixture
    norms = []
    for at in range(0, mixture.shape[1], head_dim):
        mean = jnp.sum(square[:, at : at + head_dim], axis=1, keepdims=True) * (1.0 / head_dim)
        norms.append(jnp.broadcast_to(lax.rsqrt(mean + 1e-06), (mixture.shape[0], head_dim)))
    out[...] = mixture * jnp.concatenate(norms, axis=1)


VMEM = pl.BlockSpec(memory_space=pltpu.VMEM)
HBM = pl.BlockSpec(memory_space=pltpu.HBM)


def combine(stat, other, reach, head_dim, last):
    shape = stat.shape[1:] if last else stat.shape
    return pl.pallas_call(
        functools.partial(combine_kernel, reach, head_dim, last),
        out_shape=jax.ShapeDtypeStruct(shape, F32),
        in_specs=[VMEM, VMEM],
        out_specs=VMEM,
        compiler_params=pltpu.CompilerParams(vmem_limit_bytes=1 << 20),
        name="combine",
    )(stat, other)


def per_device(tokens, key_weight, value_weight, queries, head_offset, key_bias):
    seqs, pos, width = tokens.shape
    depth, kv_width = key_weight.shape
    all_heads = head_offset.shape[0]
    head_dim = kv_width // all_heads
    tp_count, sp_count = lax.axis_size("tp"), lax.axis_size("sp")
    cols = kv_width // tp_count
    heads = all_heads // tp_count
    span = tp_count * pos
    half = sp_count // 2
    shape = jax.ShapeDtypeStruct

    def params(mib, flops=0):
        return {
            "compiler_params": pltpu.CompilerParams(vmem_limit_bytes=int(mib * 2**20)),
            "cost_estimate": pl.CostEstimate(flops=flops, bytes_accessed=0, transcendentals=0),
        }

    def shift(array, step):
        perm = [((i + step) % tp_count, i) for i in range(tp_count)]
        return lax.ppermute(array, "tp", perm)

    ring = ring_perm(sp_count)

    def onward(array):
        return lax.ppermute(array, ("gr", "sp"), ring)

    def across(array):
        return lax.ppermute(array, "gr", [(0, 1), (1, 0)])

    def stay(array):
        return pltpu.with_memory_space_constraint(array, pltpu.HBM)

    flat = tokens.reshape(seqs * pos, width)
    a = pl.pallas_call(
        functools.partial(first_kernel, cols),
        out_shape=pltpu.VMEM((depth, cols), BF16),
        in_specs=[HBM] * 2,
        out_specs=VMEM,
        scratch_shapes=[pltpu.SemaphoreType.DMA],
        name="first",
        **params(1),
    )(stay(key_weight), stay(value_weight))
    b, rows, query, offset, *biases = pl.pallas_call(
        functools.partial(second_kernel, (tp_count, heads, cols)),
        out_shape=(
            pltpu.VMEM((depth, cols), BF16),
            pltpu.VMEM((seqs * pos, width), BF16),
            pltpu.VMEM((seqs, cols), BF16),
            pltpu.VMEM((heads, pos), F32),
        )
        + (pltpu.VMEM((seqs, heads, pos), BF16),) * tp_count,
        in_specs=[HBM] * 6,
        out_specs=(VMEM,) * (4 + tp_count),
        scratch_shapes=[
            pltpu.VMEM((1, all_heads), F32),
            pltpu.VMEM((seqs, all_heads, pos), BF16),
            pltpu.SemaphoreType.DMA((5,)),
        ],
        name="second",
        **params(2),
    )(
        stay(key_weight),
        stay(value_weight),
        stay(flat),
        stay(queries),
        stay(head_offset[None]),
        stay(jnp.transpose(key_bias, (0, 2, 1))),
    )
    toks = [rows] + [shift(flat, t) for t in range(1, tp_count)]
    biases = biases[:1] + [shift(biases[t], t) for t in range(1, tp_count)]
    first, second = [a], [b]
    for _ in range(1, half):
        a, b = onward(a), onward(b)
        first += [a, across(b)]
        second += [b, across(a)]
    a = onward(a)
    first.append(a)
    second.append(across(a))

    count, early, middle = sp_count, sp_count - 3, sp_count - 1
    if depth % 128:
        places = jnp.stack(origins(range(sp_count), sp_count))
        slot_of = jnp.argmax(places[None] == lax.iota(jnp.int32, sp_count)[:, None], axis=1)
        first = [jnp.stack(first)[slot_of].reshape(width, cols)]
        second = [jnp.stack(second)[slot_of].reshape(width, cols)]
        count, early, middle = 1, 0, 0

    acc = []
    if early:
        acc = pl.pallas_call(
            functools.partial(early_kernel, early, count, depth),
            out_shape=shape((2, seqs * pos, cols), F32),
            in_specs=[VMEM] * (1 + 2 * early),
            out_specs=VMEM,
            name="early",
            **params(8, 1 << 30),
        )(rows, *first[:early], *second[:early])
        acc = pl.pallas_call(
            functools.partial(middle_kernel, tp_count, early, middle, count, depth),
            out_shape=shape((2, tp_count * seqs * pos, cols), F32),
            in_specs=[VMEM] * (1 + tp_count + 2 * middle),
            out_specs=VMEM,
            name="middle",
            **params(8, 1 << 30),
        )(acc, *toks, *first[:middle], *second[:middle])
        acc = [acc]
    slots = tuple(range(middle, len(first)))
    sizes = (tp_count, early, slots, count, seqs, pos, depth, cols, heads, head_dim)
    cache = shape((seqs, span, cols), BF16)
    bias_shape = shape((seqs, heads, span), BF16)
    keys, values, bias, stat = pl.pallas_call(
        functools.partial(attend_kernel, sizes),
        out_shape=(cache, cache, bias_shape, shape((2, seqs, cols), F32)),
        in_specs=[VMEM] * (2 + len(acc) + 2 * tp_count + 2 * len(slots)),
        out_specs=(VMEM,) * 4,
        scratch_shapes=[pltpu.VMEM((seqs * heads, span), F32)],
        name="attend",
        **params(8 if early else 32, 1 << 30),
    )(query, offset, *acc, *toks, *first[middle:], *second[middle:], *biases)
    key_cache, value_cache, bias = pl.pallas_call(
        store_kernel,
        out_shape=(cache, cache, bias_shape),
        in_specs=[VMEM] * 3,
        out_specs=(HBM,) * 3,
        scratch_shapes=[pltpu.SemaphoreType.DMA((3,))],
        name="store",
        **params(1),
    )(keys, values, bias)

    reach = 1
    while reach < sp_count:
        other = lax.ppermute(stat, "sp", [(i, i ^ reach) for i in range(sp_count)])
        stat = combine(stat, other, reach, head_dim, 2 * reach == sp_count)
        reach *= 2
    return key_cache, value_cache, jnp.transpose(bias, (0, 2, 1)), stat


def solution(mesh):
    in_specs = (
        P("gr", ("sp", "tp"), None),
        P("sp", None),
        P("sp", None),
        P("gr", None),
        P(),
        P("gr", ("sp", "tp"), None),
    )
    out_specs = (P("gr", "sp", "tp"), P("gr", "sp", "tp"), P("gr", "sp", "tp"), P("gr", "tp"))
    return jax.shard_map(
        per_device, mesh=mesh, in_specs=in_specs, out_specs=out_specs, check_vma=False
    )
```

```python
import functools

import jax
import jax.numpy as jnp
from jax import lax
from jax.experimental import pallas as pl
from jax.experimental.pallas import tpu as pltpu
from jax.sharding import PartitionSpec as P


BF16 = jnp.bfloat16
F32 = jnp.float32


def wrapped(value, count):
    value = jnp.where(value < 0, value + count, value)
    return jnp.where(value >= count, value - count, value)


def ring_perm(count):
    order = list(range(0, count, 2)) + list(range(1, count, 2))[::-1]
    pairs = []
    for p in range(count):
        here, there = order[p], order[(p + 1) % count]
        pairs.append((here, there))
        pairs.append((count + there, count + here))
    return pairs


def origins(slots, count):
    index, forward = lax.axis_index("sp"), lax.axis_index("gr") == 0
    half = lax.shift_right_logical(index, 1)
    place = jnp.where(lax.bitwise_and(index, 1) == 0, half, count - 1 - half)
    found = []
    for slot in slots:
        away = (slot + 1) // 2 * (-1 if slot % 2 == 1 else 1)
        at = wrapped(place + jnp.where(forward, away, -away), count)
        found.append(jnp.where(at < count // 2, 2 * at, 2 * (count - 1 - at) + 1))
    return found


def taken(slots, count, depth, x):
    if count == 1:
        return x[...]
    parts = []
    for at in origins(slots, count):
        at = pl.multiple_of(at * depth, depth)
        parts.append(x[:, pl.ds(at, depth)])
    return parts[0] if len(parts) == 1 else jnp.concatenate(parts, axis=1)


def stacked(refs):
    parts = [ref[...] for ref in refs]
    return parts[0] if len(parts) == 1 else jnp.concatenate(parts, axis=0)


def dot(x, w):
    return jnp.dot(x, w, preferred_element_type=F32)


def early_kernel(count, total, depth, x, *refs):
    part = taken(range(count), total, depth, x)
    for i in range(2):
        refs[2 * count][i] = dot(part, stacked(refs[i * count : (i + 1) * count]))


def middle_kernel(tp_count, early, count, total, depth, before, *refs):
    toks, refs = refs[:tp_count], refs[tp_count:]
    weights, acc = (refs[:count], refs[count : 2 * count]), refs[2 * count]
    rows = before.shape[1]
    for t in range(tp_count):
        start = early if t == 0 else 0
        if start == count:
            acc[:, :rows] = before[...]
            continue
        part = taken(range(start, count), total, depth, toks[t])
        for i in range(2):
            product = dot(part, stacked(weights[i][start:]))
            if t == 0:
                product += before[i]
            acc[i, t * rows : (t + 1) * rows] = product


def attend_kernel(sizes, query, offset, *refs):
    tp_count, early, slots, count, seqs, pos, depth, cols, heads, head_dim = sizes
    acc, refs = (refs[0], refs[1:]) if early else (None, refs)
    toks, refs = refs[:tp_count], refs[tp_count:]
    first, second = refs[: len(slots)], refs[len(slots) : 2 * len(slots)]
    biases, (keys, values, bias_out, stat_out, bias) = (
        refs[2 * len(slots) : -5],
        refs[-5:],
    )
    span = tp_count * pos
    rows = seqs * pos
    swapped = lax.axis_index("gr") != 0
    me_tp = lax.axis_index("tp")
    side = swapped.astype(jnp.int32)
    one, two = stacked(first), stacked(second)
    weights = (jnp.where(swapped, two, one), jnp.where(swapped, one, two))
    for t in range(tp_count):
        start = pl.multiple_of(wrapped(me_tp + t, tp_count) * pos, pos)
        for s in range(seqs):
            part = biases[t][s].astype(F32)
            bias[s * heads : (s + 1) * heads, pl.ds(start, pos)] = part + offset[...]
            bias_out[s, :, pl.ds(start, pos)] = biases[t][s]
    for i, (weight, target) in enumerate(zip(weights, (keys, values))):
        for t in range(tp_count):
            start = pl.multiple_of(wrapped(me_tp + t, tp_count) * pos, pos)
            product = dot(taken(slots, count, depth, toks[t]), weight)
            if early:
                product += acc[side if i == 0 else 1 - side, t * rows : (t + 1) * rows]
            for s in range(seqs):
                piece = product[s * pos : (s + 1) * pos].astype(BF16)
                target[s, pl.ds(start, pos), :] = piece
    lane_head = lax.broadcasted_iota(jnp.int32, (heads, cols), 1) // head_dim
    own_head = lane_head == lax.broadcasted_iota(jnp.int32, (heads, cols), 0)
    logits = []
    for s in range(seqs):
        q = jnp.where(own_head, jnp.broadcast_to(query[s : s + 1], (heads, cols)), 0).astype(BF16)
        logits.append(
            lax.dot_general(q, keys[s], (((1,), (1,)), ((), ())), preferred_element_type=F32)
        )
    logits = jnp.concatenate(logits, axis=0) * (head_dim**-0.5) + bias[...]
    soft = jnp.log1p(jnp.exp(-jnp.abs(logits)))
    fading = -jnp.maximum(logits, 0.0) - soft
    rising = jnp.minimum(logits, 0.0) - soft
    above = lax.broadcasted_iota(jnp.int32, (span, span), 0) > lax.broadcasted_iota(
        jnp.int32, (span, span), 1
    )
    parts, rest = [], fading
    for _ in range(3):
        parts.append(rest.astype(BF16))
        rest = rest - parts[-1].astype(F32)
    sums = dot(jnp.concatenate(parts, axis=0), jnp.where(above, 1.0, 0.0).astype(BF16))
    count = seqs * heads
    within = sums[:count] + sums[count : 2 * count] + sums[2 * count :]
    total = within[:, :1] + fading[:, :1]
    weights = jnp.exp(rising + within)
    high = weights.astype(BF16)
    low = (weights - high.astype(F32)).astype(BF16)
    for s in range(seqs):
        mine = slice(s * heads, (s + 1) * heads)
        spread = dot(jnp.concatenate([high[mine], low[mine]], axis=0), values[s])
        spread = spread[:heads] + spread[heads:]
        stat_out[0, s : s + 1] = jnp.sum(jnp.where(own_head, spread, 0.0), axis=0, keepdims=True)
        totals = jnp.where(own_head, jnp.broadcast_to(total[mine], (heads, cols)), 0.0)
        stat_out[1, s : s + 1] = jnp.sum(totals, axis=0, keepdims=True)


def first_kernel(cols, keys, values, first, second, sems):
    at = pl.ds(pl.multiple_of(lax.axis_index("tp") * cols, cols), cols)
    forward = lax.axis_index("gr") == 0

    def copies(one, two):
        return [
            pltpu.make_async_copy(one.at[:, at], first, sems.at[0]),
            pltpu.make_async_copy(two.at[:, at], second, sems.at[1]),
        ]

    ahead, back = copies(keys, values), copies(values, keys)

    @pl.when(forward)
    def _():
        for copy in ahead:
            copy.start()

    @pl.when(jnp.logical_not(forward))
    def _():
        for copy in back:
            copy.start()

    for copy in ahead:
        copy.wait()


def second_kernel(sizes, tokens, queries, offsets, biases, *refs):
    tp_count, heads, cols = sizes
    rows, query, offset = refs[:3]
    parts, (offsets_here, biases_here, sems) = refs[3:-3], refs[-3:]
    me = lax.axis_index("tp")
    at = pl.ds(pl.multiple_of(me * cols, cols), cols)
    copies = [
        pltpu.make_async_copy(biases, biases_here, sems.at[0]),
        pltpu.make_async_copy(offsets, offsets_here, sems.at[1]),
        pltpu.make_async_copy(queries.at[:, at], query, sems.at[2]),
        pltpu.make_async_copy(tokens, rows, sems.at[3]),
    ]
    for copy in copies:
        copy.start()
    copies[0].wait()
    copies[1].wait()
    shape = (heads, offsets.shape[1])
    wanted = lax.broadcasted_iota(jnp.int32, shape, 0) + me * heads
    found = lax.broadcasted_iota(jnp.int32, shape, 1) == wanted
    picked = jnp.where(found, jnp.broadcast_to(offsets_here[...], shape), 0.0)
    offset[...] = jnp.broadcast_to(jnp.sum(picked, axis=1, keepdims=True), offset.shape)
    every = biases_here[...].astype(F32)
    for t, part in enumerate(parts):
        target = wrapped(me - t, tp_count)
        chosen = every[:, :heads]
        for n in range(1, tp_count):
            chosen = jnp.where(target == n, every[:, n * heads : (n + 1) * heads], chosen)
        part[...] = chosen.astype(BF16)
    copies[2].wait()
    copies[3].wait()


def store_kernel(keys, values, bias, key_out, value_out, bias_out, sems):
    pairs = ((keys, key_out), (values, value_out), (bias, bias_out))
    copies = [pltpu.make_async_copy(a, b, sems.at[i]) for i, (a, b) in enumerate(pairs)]
    for copy in copies:
        copy.start()
    for copy in copies:
        copy.wait()


def combine_kernel(offsets, head_dim, last, *refs):
    stats, out = refs[:-1], refs[-1]
    index = lax.axis_index("sp")
    places = [lax.bitwise_xor(index, offset) for offset in offsets]
    totals = [stat[1] for stat in stats]
    mixture = None
    for i, stat in enumerate(stats):
        fade = None
        for j, total in enumerate(totals):
            if j != i:
                part = jnp.where(places[j] > places[i], total, 0.0)
                fade = part if fade is None else fade + part
        term = stat[0] * jnp.exp(fade)
        mixture = term if mixture is None else mixture + term
    if not last:
        out[0] = mixture
        out[1] = functools.reduce(jnp.add, totals)
        return
    square = mixture * mixture
    norms = []
    for at in range(0, mixture.shape[1], head_dim):
        mean = jnp.sum(square[:, at : at + head_dim], axis=1, keepdims=True) * (1.0 / head_dim)
        norms.append(jnp.broadcast_to(lax.rsqrt(mean + 1e-06), (mixture.shape[0], head_dim)))
    out[...] = mixture * jnp.concatenate(norms, axis=1)


VMEM = pl.BlockSpec(memory_space=pltpu.VMEM)
HBM = pl.BlockSpec(memory_space=pltpu.HBM)


def combine(stats, offsets, head_dim, last):
    shape = stats[0].shape[1:] if last else stats[0].shape
    return pl.pallas_call(
        functools.partial(combine_kernel, offsets, head_dim, last),
        out_shape=jax.ShapeDtypeStruct(shape, F32),
        in_specs=[VMEM] * len(stats),
        out_specs=VMEM,
        compiler_params=pltpu.CompilerParams(vmem_limit_bytes=1 << 20),
        name="combine",
    )(*stats)


def exchanges(count):
    found, reach = [], 1
    while reach < count:
        found.append((3 * reach, reach, 2 * reach) if 4 * reach <= count else (reach,))
        reach *= 4 if 4 * reach <= count else 2
    return found


def per_device(tokens, key_weight, value_weight, queries, head_offset, key_bias):
    seqs, pos, width = tokens.shape
    depth, kv_width = key_weight.shape
    all_heads = head_offset.shape[0]
    head_dim = kv_width // all_heads
    tp_count, sp_count = lax.axis_size("tp"), lax.axis_size("sp")
    cols = kv_width // tp_count
    heads = all_heads // tp_count
    span = tp_count * pos
    half = sp_count // 2
    shape = jax.ShapeDtypeStruct

    def params(mib, flops=0):
        return {
            "compiler_params": pltpu.CompilerParams(vmem_limit_bytes=int(mib * 2**20)),
            "cost_estimate": pl.CostEstimate(flops=flops, bytes_accessed=0, transcendentals=0),
        }

    def shift(array, step):
        perm = [((i + step) % tp_count, i) for i in range(tp_count)]
        return lax.ppermute(array, "tp", perm)

    ring = ring_perm(sp_count)

    def onward(array):
        return lax.ppermute(array, ("gr", "sp"), ring)

    def across(array):
        return lax.ppermute(array, "gr", [(0, 1), (1, 0)])

    def stay(array):
        return pltpu.with_memory_space_constraint(array, pltpu.HBM)

    flat = tokens.reshape(seqs * pos, width)
    a, b = pl.pallas_call(
        functools.partial(first_kernel, cols),
        out_shape=(pltpu.VMEM((depth, cols), BF16),) * 2,
        in_specs=[HBM] * 2,
        out_specs=(VMEM,) * 2,
        scratch_shapes=[pltpu.SemaphoreType.DMA((2,))],
        name="first",
        **params(1),
    )(stay(key_weight), stay(value_weight))
    rows, query, offset, *biases = pl.pallas_call(
        functools.partial(second_kernel, (tp_count, heads, cols)),
        out_shape=(
            pltpu.VMEM((seqs * pos, width), BF16),
            pltpu.VMEM((seqs, cols), BF16),
            pltpu.VMEM((heads, pos), F32),
        )
        + (pltpu.VMEM((seqs, heads, pos), BF16),) * tp_count,
        in_specs=[HBM] * 4,
        out_specs=(VMEM,) * (3 + tp_count),
        scratch_shapes=[
            pltpu.VMEM((1, all_heads), F32),
            pltpu.VMEM((seqs, all_heads, pos), BF16),
            pltpu.SemaphoreType.DMA((4,)),
        ],
        name="second",
        **params(2),
    )(stay(flat), stay(queries), stay(head_offset[None]), stay(jnp.transpose(key_bias, (0, 2, 1))))
    toks = [rows] + [shift(flat, t) for t in range(1, tp_count)]
    biases = biases[:1] + [shift(biases[t], t) for t in range(1, tp_count)]
    first, second = [a], [b]
    for _ in range(1, half):
        a, b = onward(a), onward(b)
        first += [a, across(b)]
        second += [b, across(a)]
    a = onward(a)
    first.append(a)
    second.append(across(a))

    count, early, middle = sp_count, sp_count - 1, sp_count - 1
    if depth % 128:
        places = jnp.stack(origins(range(sp_count), sp_count))
        slot_of = jnp.argmax(places[None] == lax.iota(jnp.int32, sp_count)[:, None], axis=1)
        first = [jnp.stack(first)[slot_of].reshape(width, cols)]
        second = [jnp.stack(second)[slot_of].reshape(width, cols)]
        count, early, middle = 1, 0, 0

    acc = []
    if early:
        acc = pl.pallas_call(
            functools.partial(early_kernel, early, count, depth),
            out_shape=shape((2, seqs * pos, cols), F32),
            in_specs=[VMEM] * (1 + 2 * early),
            out_specs=VMEM,
            name="early",
            **params(8, 1 << 30),
        )(rows, *first[:early], *second[:early])
        acc = pl.pallas_call(
            functools.partial(middle_kernel, tp_count, early, middle, count, depth),
            out_shape=shape((2, tp_count * seqs * pos, cols), F32),
            in_specs=[VMEM] * (1 + tp_count + 2 * middle),
            out_specs=VMEM,
            name="middle",
            **params(8, 1 << 30),
        )(acc, *toks, *first[:middle], *second[:middle])
        acc = [acc]
    slots = tuple(range(middle, len(first)))
    sizes = (tp_count, early, slots, count, seqs, pos, depth, cols, heads, head_dim)
    cache = shape((seqs, span, cols), BF16)
    bias_shape = shape((seqs, heads, span), BF16)
    keys, values, bias, stat = pl.pallas_call(
        functools.partial(attend_kernel, sizes),
        out_shape=(cache, cache, bias_shape, shape((2, seqs, cols), F32)),
        in_specs=[VMEM] * (2 + len(acc) + 2 * tp_count + 2 * len(slots)),
        out_specs=(VMEM,) * 4,
        scratch_shapes=[pltpu.VMEM((seqs * heads, span), F32)],
        name="attend",
        **params(8 if early else 32, 1 << 30),
    )(query, offset, *acc, *toks, *first[middle:], *second[middle:], *biases)
    key_cache, value_cache, bias = pl.pallas_call(
        store_kernel,
        out_shape=(cache, cache, bias_shape),
        in_specs=[VMEM] * 3,
        out_specs=(HBM,) * 3,
        scratch_shapes=[pltpu.SemaphoreType.DMA((3,))],
        name="store",
        **params(1),
    )(keys, values, bias)

    stages = exchanges(sp_count)
    for n, offsets in enumerate(stages):
        stats = [stat]
        for offset in offsets:
            perm = [(i, i ^ offset) for i in range(sp_count)]
            stats.append(lax.ppermute(stat, "sp", perm))
        stat = combine(stats, (0,) + offsets, head_dim, n + 1 == len(stages))
    return key_cache, value_cache, jnp.transpose(bias, (0, 2, 1)), stat


def solution(mesh):
    in_specs = (
        P("gr", ("sp", "tp"), None),
        P("sp", None),
        P("sp", None),
        P("gr", None),
        P(),
        P("gr", ("sp", "tp"), None),
    )
    out_specs = (P("gr", "sp", "tp"), P("gr", "sp", "tp"), P("gr", "sp", "tp"), P("gr", "tp"))
    return jax.shard_map(
        per_device, mesh=mesh, in_specs=in_specs, out_specs=out_specs, check_vma=False
    )
```

```python
import functools

import jax
import jax.numpy as jnp
from jax import lax
from jax.experimental import pallas as pl
from jax.experimental.pallas import tpu as pltpu
from jax.sharding import PartitionSpec as P


BF16 = jnp.bfloat16
F32 = jnp.float32


def wrapped(value, count):
    value = jnp.where(value < 0, value + count, value)
    return jnp.where(value >= count, value - count, value)


def ring_perm(count):
    order = list(range(0, count, 2)) + list(range(1, count, 2))[::-1]
    pairs = []
    for p in range(count):
        here, there = order[p], order[(p + 1) % count]
        pairs.append((here, there))
        pairs.append((count + there, count + here))
    return pairs


def origins(slots, count):
    index, forward = lax.axis_index("sp"), lax.axis_index("gr") == 0
    half = lax.shift_right_logical(index, 1)
    place = jnp.where(lax.bitwise_and(index, 1) == 0, half, count - 1 - half)
    found = []
    for slot in slots:
        away = (slot + 1) // 2 * (-1 if slot % 2 == 1 else 1)
        at = wrapped(place + jnp.where(forward, away, -away), count)
        found.append(jnp.where(at < count // 2, 2 * at, 2 * (count - 1 - at) + 1))
    return found


def taken(slots, count, depth, x):
    if count == 1:
        return x[...]
    parts = []
    for at in origins(slots, count):
        at = pl.multiple_of(at * depth, depth)
        parts.append(x[:, pl.ds(at, depth)])
    return parts[0] if len(parts) == 1 else jnp.concatenate(parts, axis=1)


def stacked(refs):
    parts = [ref[...] for ref in refs]
    return parts[0] if len(parts) == 1 else jnp.concatenate(parts, axis=0)


def dot(x, w):
    return jnp.dot(x, w, preferred_element_type=F32)


def early_kernel(count, total, depth, x, *refs):
    part = taken(range(count), total, depth, x)
    for i in range(2):
        refs[2 * count][i] = dot(part, stacked(refs[i * count : (i + 1) * count]))


def middle_kernel(tp_count, early, count, total, depth, before, *refs):
    toks, refs = refs[:tp_count], refs[tp_count:]
    weights, acc = (refs[:count], refs[count : 2 * count]), refs[2 * count]
    rows = before.shape[1]
    for t in range(tp_count):
        start = early if t == 0 else 0
        if start == count:
            acc[:, :rows] = before[...]
            continue
        part = taken(range(start, count), total, depth, toks[t])
        for i in range(2):
            product = dot(part, stacked(weights[i][start:]))
            if t == 0:
                product += before[i]
            acc[i, t * rows : (t + 1) * rows] = product


def attend_kernel(sizes, query, offset, *refs):
    tp_count, early, slots, count, seqs, pos, depth, cols, heads, head_dim = sizes
    acc, refs = (refs[0], refs[1:]) if early else (None, refs)
    toks, refs = refs[:tp_count], refs[tp_count:]
    first, second = refs[: len(slots)], refs[len(slots) : 2 * len(slots)]
    biases, (keys, values, bias_out, stat_out, bias) = (
        refs[2 * len(slots) : -5],
        refs[-5:],
    )
    span = tp_count * pos
    rows = seqs * pos
    swapped = lax.axis_index("gr") != 0
    me_tp = lax.axis_index("tp")
    side = swapped.astype(jnp.int32)
    one, two = stacked(first), stacked(second)
    weights = (jnp.where(swapped, two, one), jnp.where(swapped, one, two))
    for t in range(tp_count):
        start = pl.multiple_of(wrapped(me_tp + t, tp_count) * pos, pos)
        for s in range(seqs):
            part = biases[t][s].astype(F32)
            bias[s * heads : (s + 1) * heads, pl.ds(start, pos)] = part + offset[...]
            bias_out[s, :, pl.ds(start, pos)] = biases[t][s]
    for i, (weight, target) in enumerate(zip(weights, (keys, values))):
        for t in range(tp_count):
            start = pl.multiple_of(wrapped(me_tp + t, tp_count) * pos, pos)
            product = dot(taken(slots, count, depth, toks[t]), weight)
            if early:
                product += acc[side if i == 0 else 1 - side, t * rows : (t + 1) * rows]
            for s in range(seqs):
                piece = product[s * pos : (s + 1) * pos].astype(BF16)
                target[s, pl.ds(start, pos), :] = piece
    lane_head = lax.broadcasted_iota(jnp.int32, (heads, cols), 1) // head_dim
    own_head = lane_head == lax.broadcasted_iota(jnp.int32, (heads, cols), 0)
    logits = []
    for s in range(seqs):
        q = jnp.where(own_head, jnp.broadcast_to(query[s : s + 1], (heads, cols)), 0).astype(BF16)
        logits.append(
            lax.dot_general(q, keys[s], (((1,), (1,)), ((), ())), preferred_element_type=F32)
        )
    logits = jnp.concatenate(logits, axis=0) * (head_dim**-0.5) + bias[...]
    soft = jnp.log1p(jnp.exp(-jnp.abs(logits)))
    fading = -jnp.maximum(logits, 0.0) - soft
    rising = jnp.minimum(logits, 0.0) - soft
    above = lax.broadcasted_iota(jnp.int32, (span, span), 0) > lax.broadcasted_iota(
        jnp.int32, (span, span), 1
    )
    parts, rest = [], fading
    for _ in range(3):
        parts.append(rest.astype(BF16))
        rest = rest - parts[-1].astype(F32)
    sums = dot(jnp.concatenate(parts, axis=0), jnp.where(above, 1.0, 0.0).astype(BF16))
    count = seqs * heads
    within = sums[:count] + sums[count : 2 * count] + sums[2 * count :]
    total = within[:, :1] + fading[:, :1]
    weights = jnp.exp(rising + within)
    high = weights.astype(BF16)
    low = (weights - high.astype(F32)).astype(BF16)
    for s in range(seqs):
        mine = slice(s * heads, (s + 1) * heads)
        spread = dot(jnp.concatenate([high[mine], low[mine]], axis=0), values[s])
        spread = spread[:heads] + spread[heads:]
        stat_out[0, s : s + 1] = jnp.sum(jnp.where(own_head, spread, 0.0), axis=0, keepdims=True)
        totals = jnp.where(own_head, jnp.broadcast_to(total[mine], (heads, cols)), 0.0)
        stat_out[1, s : s + 1] = jnp.sum(totals, axis=0, keepdims=True)


def first_kernel(cols, keys, values, first, second, sems):
    at = pl.ds(pl.multiple_of(lax.axis_index("tp") * cols, cols), cols)
    forward = lax.axis_index("gr") == 0

    def copies(one, two):
        return [
            pltpu.make_async_copy(one.at[:, at], first, sems.at[0]),
            pltpu.make_async_copy(two.at[:, at], second, sems.at[1]),
        ]

    ahead, back = copies(keys, values), copies(values, keys)

    @pl.when(forward)
    def _():
        for copy in ahead:
            copy.start()

    @pl.when(jnp.logical_not(forward))
    def _():
        for copy in back:
            copy.start()

    for copy in ahead:
        copy.wait()


def second_kernel(sizes, tokens, queries, offsets, biases, *refs):
    tp_count, heads, cols = sizes
    rows, query, offset = refs[:3]
    parts, (offsets_here, biases_here, sems) = refs[3:-3], refs[-3:]
    me = lax.axis_index("tp")
    at = pl.ds(pl.multiple_of(me * cols, cols), cols)
    copies = [
        pltpu.make_async_copy(biases, biases_here, sems.at[0]),
        pltpu.make_async_copy(offsets, offsets_here, sems.at[1]),
        pltpu.make_async_copy(queries.at[:, at], query, sems.at[2]),
        pltpu.make_async_copy(tokens, rows, sems.at[3]),
    ]
    for copy in copies:
        copy.start()
    copies[0].wait()
    copies[1].wait()
    shape = (heads, offsets.shape[1])
    wanted = lax.broadcasted_iota(jnp.int32, shape, 0) + me * heads
    found = lax.broadcasted_iota(jnp.int32, shape, 1) == wanted
    picked = jnp.where(found, jnp.broadcast_to(offsets_here[...], shape), 0.0)
    offset[...] = jnp.broadcast_to(jnp.sum(picked, axis=1, keepdims=True), offset.shape)
    every = biases_here[...].astype(F32)
    for t, part in enumerate(parts):
        target = wrapped(me - t, tp_count)
        chosen = every[:, :heads]
        for n in range(1, tp_count):
            chosen = jnp.where(target == n, every[:, n * heads : (n + 1) * heads], chosen)
        part[...] = chosen.astype(BF16)
    copies[2].wait()
    copies[3].wait()


def store_kernel(keys, values, bias, key_out, value_out, bias_out, sems):
    pairs = ((keys, key_out), (values, value_out), (bias, bias_out))
    copies = [pltpu.make_async_copy(a, b, sems.at[i]) for i, (a, b) in enumerate(pairs)]
    for copy in copies:
        copy.start()
    for copy in copies:
        copy.wait()


def combine_kernel(offsets, head_dim, last, *refs):
    stats, out = refs[:-1], refs[-1]
    index = lax.axis_index("sp")
    places = [lax.bitwise_xor(index, offset) for offset in offsets]
    totals = [stat[1] for stat in stats]
    mixture = None
    for i, stat in enumerate(stats):
        fade = None
        for j, total in enumerate(totals):
            if j != i:
                part = jnp.where(places[j] > places[i], total, 0.0)
                fade = part if fade is None else fade + part
        term = stat[0] * jnp.exp(fade)
        mixture = term if mixture is None else mixture + term
    if not last:
        out[0] = mixture
        out[1] = functools.reduce(jnp.add, totals)
        return
    square = mixture * mixture
    norms = []
    for at in range(0, mixture.shape[1], head_dim):
        mean = jnp.sum(square[:, at : at + head_dim], axis=1, keepdims=True) * (1.0 / head_dim)
        norms.append(jnp.broadcast_to(lax.rsqrt(mean + 1e-06), (mixture.shape[0], head_dim)))
    out[...] = mixture * jnp.concatenate(norms, axis=1)


VMEM = pl.BlockSpec(memory_space=pltpu.VMEM)
HBM = pl.BlockSpec(memory_space=pltpu.HBM)


def combine(stats, offsets, head_dim, last):
    shape = stats[0].shape[1:] if last else stats[0].shape
    return pl.pallas_call(
        functools.partial(combine_kernel, offsets, head_dim, last),
        out_shape=jax.ShapeDtypeStruct(shape, F32),
        in_specs=[VMEM] * len(stats),
        out_specs=VMEM,
        compiler_params=pltpu.CompilerParams(vmem_limit_bytes=1 << 20),
        name="combine",
    )(*stats)


def exchanges(count):
    found, reach = [], 1
    while reach < count:
        found.append((3 * reach, reach, 2 * reach) if 4 * reach <= count else (reach,))
        reach *= 4 if 4 * reach <= count else 2
    return found


def per_device(tokens, key_weight, value_weight, queries, head_offset, key_bias):
    seqs, pos, width = tokens.shape
    depth, kv_width = key_weight.shape
    all_heads = head_offset.shape[0]
    head_dim = kv_width // all_heads
    tp_count, sp_count = lax.axis_size("tp"), lax.axis_size("sp")
    cols = kv_width // tp_count
    heads = all_heads // tp_count
    span = tp_count * pos
    half = sp_count // 2
    shape = jax.ShapeDtypeStruct

    def params(mib, flops=0):
        return {
            "compiler_params": pltpu.CompilerParams(vmem_limit_bytes=int(mib * 2**20)),
            "cost_estimate": pl.CostEstimate(flops=flops, bytes_accessed=0, transcendentals=0),
        }

    def shift(array, step):
        perm = [((i + step) % tp_count, i) for i in range(tp_count)]
        return lax.ppermute(array, "tp", perm)

    ring = ring_perm(sp_count)

    def onward(array):
        return lax.ppermute(array, ("gr", "sp"), ring)

    def across(array):
        return lax.ppermute(array, "gr", [(0, 1), (1, 0)])

    def stay(array):
        return pltpu.with_memory_space_constraint(array, pltpu.HBM)

    flat = tokens.reshape(seqs * pos, width)
    a, b = pl.pallas_call(
        functools.partial(first_kernel, cols),
        out_shape=(pltpu.VMEM((depth, cols), BF16),) * 2,
        in_specs=[HBM] * 2,
        out_specs=(VMEM,) * 2,
        scratch_shapes=[pltpu.SemaphoreType.DMA((2,))],
        name="first",
        **params(1),
    )(stay(key_weight), stay(value_weight))
    rows, query, offset, *biases = pl.pallas_call(
        functools.partial(second_kernel, (tp_count, heads, cols)),
        out_shape=(
            pltpu.VMEM((seqs * pos, width), BF16),
            pltpu.VMEM((seqs, cols), BF16),
            pltpu.VMEM((heads, pos), F32),
        )
        + (pltpu.VMEM((seqs, heads, pos), BF16),) * tp_count,
        in_specs=[HBM] * 4,
        out_specs=(VMEM,) * (3 + tp_count),
        scratch_shapes=[
            pltpu.VMEM((1, all_heads), F32),
            pltpu.VMEM((seqs, all_heads, pos), BF16),
            pltpu.SemaphoreType.DMA((4,)),
        ],
        name="second",
        **params(2),
    )(stay(flat), stay(queries), stay(head_offset[None]), stay(jnp.transpose(key_bias, (0, 2, 1))))
    toks = [rows] + [shift(flat, t) for t in range(1, tp_count)]
    biases = biases[:1] + [shift(biases[t], t) for t in range(1, tp_count)]
    first, second = [a], [b]
    for _ in range(1, half):
        a, b = onward(a), onward(b)
        first += [a, across(b)]
        second += [b, across(a)]
    a = onward(a)
    first.append(a)
    second.append(across(a))

    count, early, middle = sp_count, sp_count - 1, sp_count - 1
    if depth % 128:
        places = jnp.stack(origins(range(sp_count), sp_count))
        slot_of = jnp.argmax(places[None] == lax.iota(jnp.int32, sp_count)[:, None], axis=1)
        first = [jnp.stack(first)[slot_of].reshape(width, cols)]
        second = [jnp.stack(second)[slot_of].reshape(width, cols)]
        count, early, middle = 1, 0, 0

    acc = []
    if early:
        acc = pl.pallas_call(
            functools.partial(early_kernel, early, count, depth),
            out_shape=shape((2, seqs * pos, cols), F32),
            in_specs=[VMEM] * (1 + 2 * early),
            out_specs=VMEM,
            name="early",
            **params(8, 1 << 30),
        )(rows, *first[:early], *second[:early])
        acc = pl.pallas_call(
            functools.partial(middle_kernel, tp_count, early, middle, count, depth),
            out_shape=shape((2, tp_count * seqs * pos, cols), F32),
            in_specs=[VMEM] * (1 + tp_count + 2 * middle),
            out_specs=VMEM,
            name="middle",
            **params(8, 1 << 30),
        )(acc, *toks, *first[:middle], *second[:middle])
        acc = [acc]
    slots = tuple(range(middle, len(first)))
    sizes = (tp_count, early, slots, count, seqs, pos, depth, cols, heads, head_dim)
    cache = shape((seqs, span, cols), BF16)
    bias_shape = shape((seqs, heads, span), BF16)
    keys, values, bias, stat = pl.pallas_call(
        functools.partial(attend_kernel, sizes),
        out_shape=(cache, cache, bias_shape, shape((2, seqs, cols), F32)),
        in_specs=[VMEM] * (2 + len(acc) + 2 * tp_count + 2 * len(slots)),
        out_specs=(VMEM,) * 4,
        scratch_shapes=[pltpu.VMEM((seqs * heads, span), F32)],
        name="attend",
        **params(8 if early else 32, 1 << 30),
    )(query, offset, *acc, *toks, *first[middle:], *second[middle:], *biases)
    key_cache, value_cache, bias = pl.pallas_call(
        store_kernel,
        out_shape=(cache, cache, bias_shape),
        in_specs=[VMEM] * 3,
        out_specs=(HBM,) * 3,
        scratch_shapes=[pltpu.SemaphoreType.DMA((3,))],
        name="store",
        **params(1),
    )(keys, values, bias)

    stages = exchanges(sp_count)
    for n, offsets in enumerate(stages):
        crossing = n < len(stages) // 2 * 2
        stats = [] if crossing else [stat]
        offsets = ((0,) if crossing else ()) + offsets
        for offset in offsets:
            perm = [
                (g * sp_count + i, (1 - g if crossing else g) * sp_count + (i ^ offset))
                for g in range(2)
                for i in range(sp_count)
            ]
            stats.append(lax.ppermute(stat, ("gr", "sp"), perm))
        offsets = offsets if crossing else (0,) + offsets
        stat = combine(stats, offsets, head_dim, n + 1 == len(stages))
    return key_cache, value_cache, jnp.transpose(bias, (0, 2, 1)), stat


def solution(mesh):
    in_specs = (
        P("gr", ("sp", "tp"), None),
        P("sp", None),
        P("sp", None),
        P("gr", None),
        P(),
        P("gr", ("sp", "tp"), None),
    )
    out_specs = (P("gr", "sp", "tp"), P("gr", "sp", "tp"), P("gr", "sp", "tp"), P("gr", "tp"))
    return jax.shard_map(
        per_device, mesh=mesh, in_specs=in_specs, out_specs=out_specs, check_vma=False
    )
```

```python
import functools

import jax
import jax.numpy as jnp
from jax import lax
from jax.experimental import pallas as pl
from jax.experimental.pallas import tpu as pltpu
from jax.sharding import PartitionSpec as P


BF16 = jnp.bfloat16
F32 = jnp.float32


def wrapped(value, count):
    value = jnp.where(value < 0, value + count, value)
    return jnp.where(value >= count, value - count, value)


def ring_perm(count, step):
    order = list(range(0, count, 2)) + list(range(1, count, 2))[::-1]
    one, two = (step - 1) % 2 * count, step % 2 * count
    pairs = []
    for p in range(count):
        here, there = order[p], order[(p + 1) % count]
        pairs.append((one + here, two + there))
        pairs.append((two + there, one + here))
    return pairs


def origins(slots, count):
    index, forward = lax.axis_index("sp"), lax.axis_index("gr") == 0
    half = lax.shift_right_logical(index, 1)
    place = jnp.where(lax.bitwise_and(index, 1) == 0, half, count - 1 - half)
    found = []
    for slot in slots:
        step = (slot + 1) // 2
        away = step if (slot + step) % 2 == 0 else -step
        at = wrapped(place + jnp.where(forward, away, -away), count)
        found.append(jnp.where(at < count // 2, 2 * at, 2 * (count - 1 - at) + 1))
    return found


def taken(slots, count, depth, x):
    if count == 1:
        return x[...]
    parts = []
    for at in origins(slots, count):
        at = pl.multiple_of(at * depth, depth)
        parts.append(x[:, pl.ds(at, depth)])
    return parts[0] if len(parts) == 1 else jnp.concatenate(parts, axis=1)


def stacked(refs):
    parts = [ref[...] for ref in refs]
    return parts[0] if len(parts) == 1 else jnp.concatenate(parts, axis=0)


def dot(x, w):
    return jnp.dot(x, w, preferred_element_type=F32)


def project_kernel(tok_count, count, total, depth, *refs):
    toks, refs = refs[:tok_count], refs[tok_count:]
    part = jnp.concatenate([taken(range(count), total, depth, tok) for tok in toks], axis=0)
    for i in range(2):
        refs[2 * count][i] = dot(part, stacked(refs[i * count : (i + 1) * count]))


def attend_kernel(sizes, query, offset, *refs):
    tp_count, early, slots, count, seqs, pos, depth, cols, heads, head_dim = sizes
    acc_count = 1 + (tp_count - 1) * seqs if early else 0
    accs, refs = refs[:acc_count], refs[acc_count:]
    toks, refs = refs[: tp_count * seqs], refs[tp_count * seqs :]
    first, second = refs[: len(slots)], refs[len(slots) : 2 * len(slots)]
    biases, (keys, values, bias_out, stat_out, bias) = (
        refs[2 * len(slots) : -5],
        refs[-5:],
    )
    span = tp_count * pos
    swapped = lax.axis_index("gr") != 0
    me_tp = lax.axis_index("tp")
    side = swapped.astype(jnp.int32)
    one, two = stacked(first), stacked(second)
    weights = (jnp.where(swapped, two, one), jnp.where(swapped, one, two))
    for t in range(tp_count):
        start = pl.multiple_of(wrapped(me_tp + t, tp_count) * pos, pos)
        for s in range(seqs):
            part = biases[t][s].astype(F32)
            bias[s * heads : (s + 1) * heads, pl.ds(start, pos)] = part + offset[...]
            bias_out[s, :, pl.ds(start, pos)] = biases[t][s]
    for i, (weight, target) in enumerate(zip(weights, (keys, values))):
        for t in range(tp_count):
            start = pl.multiple_of(wrapped(me_tp + t, tp_count) * pos, pos)
            parts = [taken(slots, count, depth, tok) for tok in toks[t * seqs : (t + 1) * seqs]]
            product = dot(jnp.concatenate(parts, axis=0), weight)
            at = side if i == 0 else 1 - side
            for s in range(seqs):
                piece = product[s * pos : (s + 1) * pos]
                if early and t == 0:
                    piece += accs[0][at, s * pos : (s + 1) * pos]
                elif early:
                    piece += accs[1 + (t - 1) * seqs + s][at]
                target[s, pl.ds(start, pos), :] = piece.astype(BF16)
    lane_head = lax.broadcasted_iota(jnp.int32, (heads, cols), 1) // head_dim
    own_head = lane_head == lax.broadcasted_iota(jnp.int32, (heads, cols), 0)
    logits = []
    for s in range(seqs):
        q = jnp.where(own_head, jnp.broadcast_to(query[s : s + 1], (heads, cols)), 0).astype(BF16)
        logits.append(
            lax.dot_general(q, keys[s], (((1,), (1,)), ((), ())), preferred_element_type=F32)
        )
    logits = jnp.concatenate(logits, axis=0) * (head_dim**-0.5) + bias[...]
    soft = jnp.log1p(jnp.exp(-jnp.abs(logits)))
    fading = -jnp.maximum(logits, 0.0) - soft
    rising = jnp.minimum(logits, 0.0) - soft
    above = lax.broadcasted_iota(jnp.int32, (span, span), 0) > lax.broadcasted_iota(
        jnp.int32, (span, span), 1
    )
    parts, rest = [], fading
    for _ in range(3):
        parts.append(rest.astype(BF16))
        rest = rest - parts[-1].astype(F32)
    sums = dot(jnp.concatenate(parts, axis=0), jnp.where(above, 1.0, 0.0).astype(BF16))
    count = seqs * heads
    within = sums[:count] + sums[count : 2 * count] + sums[2 * count :]
    total = within[:, :1] + fading[:, :1]
    weights = jnp.exp(rising + within)
    high = weights.astype(BF16)
    low = (weights - high.astype(F32)).astype(BF16)
    for s in range(seqs):
        mine = slice(s * heads, (s + 1) * heads)
        spread = dot(jnp.concatenate([high[mine], low[mine]], axis=0), values[s])
        spread = spread[:heads] + spread[heads:]
        stat_out[0, s : s + 1] = jnp.sum(jnp.where(own_head, spread, 0.0), axis=0, keepdims=True)
        totals = jnp.where(own_head, jnp.broadcast_to(total[mine], (heads, cols)), 0.0)
        stat_out[1, s : s + 1] = jnp.sum(totals, axis=0, keepdims=True)


def first_kernel(cols, keys, values, tokens, first, second, *refs):
    rows, sems = refs
    at = pl.ds(pl.multiple_of(lax.axis_index("tp") * cols, cols), cols)
    forward = lax.axis_index("gr") == 0

    def copies(one, two):
        return [
            pltpu.make_async_copy(one.at[:, at], first, sems.at[0]),
            pltpu.make_async_copy(two.at[:, at], second, sems.at[1]),
        ]

    ahead, back = copies(keys, values), copies(values, keys)
    tokens_in = pltpu.make_async_copy(tokens.at[0], rows, sems.at[2])

    @pl.when(forward)
    def _():
        for copy in ahead:
            copy.start()

    @pl.when(jnp.logical_not(forward))
    def _():
        for copy in back:
            copy.start()

    tokens_in.start()
    for copy in ahead:
        copy.wait()
    tokens_in.wait()


def second_kernel(sizes, tokens, queries, offsets, biases, *refs):
    tp_count, heads, cols = sizes
    query, offset = refs[:2]
    rows, refs = refs[2 : 1 + tokens.shape[0]], refs[1 + tokens.shape[0] :]
    parts, (offsets_here, biases_here, sems) = refs[:-3], refs[-3:]
    me = lax.axis_index("tp")
    at = pl.ds(pl.multiple_of(me * cols, cols), cols)
    copies = [
        pltpu.make_async_copy(biases, biases_here, sems.at[0]),
        pltpu.make_async_copy(offsets, offsets_here, sems.at[1]),
        pltpu.make_async_copy(queries.at[:, at], query, sems.at[2]),
    ] + [
        pltpu.make_async_copy(tokens.at[s + 1], row, sems.at[3 + s]) for s, row in enumerate(rows)
    ]
    for copy in copies:
        copy.start()
    copies[0].wait()
    copies[1].wait()
    shape = (heads, offsets.shape[1])
    wanted = lax.broadcasted_iota(jnp.int32, shape, 0) + me * heads
    found = lax.broadcasted_iota(jnp.int32, shape, 1) == wanted
    picked = jnp.where(found, jnp.broadcast_to(offsets_here[...], shape), 0.0)
    offset[...] = jnp.broadcast_to(jnp.sum(picked, axis=1, keepdims=True), offset.shape)
    every = biases_here[...].astype(F32)
    for t, part in enumerate(parts):
        target = wrapped(me - t, tp_count)
        chosen = every[:, :heads]
        for n in range(1, tp_count):
            chosen = jnp.where(target == n, every[:, n * heads : (n + 1) * heads], chosen)
        part[...] = chosen.astype(BF16)
    for copy in copies[2:]:
        copy.wait()


def store_kernel(keys, values, bias, key_out, value_out, bias_out, sems):
    pairs = ((keys, key_out), (values, value_out), (bias, bias_out))
    copies = [pltpu.make_async_copy(a, b, sems.at[i]) for i, (a, b) in enumerate(pairs)]
    for copy in copies:
        copy.start()
    for copy in copies:
        copy.wait()


def combine_kernel(offsets, head_dim, last, *refs):
    stats, out = refs[:-1], refs[-1]
    index = lax.axis_index("sp")
    places = [lax.bitwise_xor(index, offset) for offset in offsets]
    totals = [stat[1] for stat in stats]
    mixture = None
    for i, stat in enumerate(stats):
        fade = None
        for j, total in enumerate(totals):
            if j != i:
                part = jnp.where(places[j] > places[i], total, 0.0)
                fade = part if fade is None else fade + part
        term = stat[0] * jnp.exp(fade)
        mixture = term if mixture is None else mixture + term
    if not last:
        out[0] = mixture
        out[1] = functools.reduce(jnp.add, totals)
        return
    square = mixture * mixture
    norms = []
    for at in range(0, mixture.shape[1], head_dim):
        mean = jnp.sum(square[:, at : at + head_dim], axis=1, keepdims=True) * (1.0 / head_dim)
        norms.append(jnp.broadcast_to(lax.rsqrt(mean + 1e-06), (mixture.shape[0], head_dim)))
    out[...] = mixture * jnp.concatenate(norms, axis=1)


VMEM = pl.BlockSpec(memory_space=pltpu.VMEM)
HBM = pl.BlockSpec(memory_space=pltpu.HBM)


def combine(stats, offsets, head_dim, last):
    shape = stats[0].shape[1:] if last else stats[0].shape
    return pl.pallas_call(
        functools.partial(combine_kernel, offsets, head_dim, last),
        out_shape=jax.ShapeDtypeStruct(shape, F32),
        in_specs=[VMEM] * len(stats),
        out_specs=VMEM,
        compiler_params=pltpu.CompilerParams(vmem_limit_bytes=1 << 20),
        name="combine",
    )(*stats)


def exchanges(count):
    found, reach = [], 1
    while reach < count:
        found.append((3 * reach, reach, 2 * reach) if 4 * reach <= count else (reach,))
        reach *= 4 if 4 * reach <= count else 2
    return found


def per_device(tokens, key_weight, value_weight, queries, head_offset, key_bias):
    seqs, pos, width = tokens.shape
    depth, kv_width = key_weight.shape
    all_heads = head_offset.shape[0]
    head_dim = kv_width // all_heads
    tp_count, sp_count = lax.axis_size("tp"), lax.axis_size("sp")
    cols = kv_width // tp_count
    heads = all_heads // tp_count
    span = tp_count * pos
    half = sp_count // 2
    shape = jax.ShapeDtypeStruct

    def params(mib, flops=0):
        return {
            "compiler_params": pltpu.CompilerParams(vmem_limit_bytes=int(mib * 2**20)),
            "cost_estimate": pl.CostEstimate(flops=flops, bytes_accessed=0, transcendentals=0),
        }

    def shift(array, step):
        perm = [((i + step) % tp_count, i) for i in range(tp_count)]
        return lax.ppermute(array, "tp", perm)

    def onward(array, step):
        return lax.ppermute(array, ("gr", "sp"), ring_perm(sp_count, step))

    def across(array):
        return lax.ppermute(array, "gr", [(0, 1), (1, 0)])

    def stay(array):
        return pltpu.with_memory_space_constraint(array, pltpu.HBM)

    a, b, row = pl.pallas_call(
        functools.partial(first_kernel, cols),
        out_shape=(pltpu.VMEM((depth, cols), BF16),) * 2 + (pltpu.VMEM((pos, width), BF16),),
        in_specs=[HBM] * 3,
        out_specs=(VMEM,) * 3,
        scratch_shapes=[pltpu.SemaphoreType.DMA((3,))],
        name="first",
        **params(1),
    )(stay(key_weight), stay(value_weight), stay(tokens))
    query, offset, *found = pl.pallas_call(
        functools.partial(second_kernel, (tp_count, heads, cols)),
        out_shape=(
            pltpu.VMEM((seqs, cols), BF16),
            pltpu.VMEM((heads, pos), F32),
        )
        + (pltpu.VMEM((pos, width), BF16),) * (seqs - 1)
        + (pltpu.VMEM((seqs, heads, pos), BF16),) * tp_count,
        in_specs=[HBM] * 4,
        out_specs=(VMEM,) * (1 + seqs + tp_count),
        scratch_shapes=[
            pltpu.VMEM((1, all_heads), F32),
            pltpu.VMEM((seqs, all_heads, pos), BF16),
            pltpu.SemaphoreType.DMA((2 + seqs,)),
        ],
        name="second",
        **params(2),
    )(
        stay(tokens),
        stay(queries),
        stay(head_offset[None]),
        stay(jnp.transpose(key_bias, (0, 2, 1))),
    )
    rows, biases = [row] + found[: seqs - 1], found[seqs - 1 :]
    toks = [rows] + [[shift(row, t) for row in rows] for t in range(1, tp_count)]
    biases = biases[:1] + [shift(biases[t], t) for t in range(1, tp_count)]
    first, second = [a], [b]
    for j in range(1, half):
        a, b = onward(a, j), onward(b, j)
        from_a, from_b = across(a), across(b)
        first += [b, from_a] if j % 2 else [a, from_b]
        second += [a, from_b] if j % 2 else [b, from_a]
    a = onward(a, half)
    from_a = across(a)
    first.append(from_a if half % 2 else a)
    second.append(a if half % 2 else from_a)

    count, early, middle = sp_count, sp_count - 1, sp_count - 1
    if depth % 128:
        places = jnp.stack(origins(range(sp_count), sp_count))
        slot_of = jnp.argmax(places[None] == lax.iota(jnp.int32, sp_count)[:, None], axis=1)
        first = [jnp.stack(first)[slot_of].reshape(width, cols)]
        second = [jnp.stack(second)[slot_of].reshape(width, cols)]
        count, early, middle = 1, 0, 0

    def project(pieces):
        return pl.pallas_call(
            functools.partial(project_kernel, len(pieces), early, count, depth),
            out_shape=shape((2, len(pieces) * pos, cols), F32),
            in_specs=[VMEM] * (len(pieces) + 2 * early),
            out_specs=VMEM,
            name="project",
            **params(8, 1 << 30),
        )(*pieces, *first[:early], *second[:early])

    accs = []
    if early:
        accs.append(project(toks[0]))
        for t in range(1, tp_count):
            accs += [project([tok]) for tok in toks[t]]
    slots = tuple(range(middle, len(first)))
    sizes = (tp_count, early, slots, count, seqs, pos, depth, cols, heads, head_dim)
    cache = shape((seqs, span, cols), BF16)
    bias_shape = shape((seqs, heads, span), BF16)
    keys, values, bias, stat = pl.pallas_call(
        functools.partial(attend_kernel, sizes),
        out_shape=(cache, cache, bias_shape, shape((2, seqs, cols), F32)),
        in_specs=[VMEM] * (2 + len(accs) + (1 + seqs) * tp_count + 2 * len(slots)),
        out_specs=(VMEM,) * 4,
        scratch_shapes=[pltpu.VMEM((seqs * heads, span), F32)],
        name="attend",
        **params(8 if early else 32, 1 << 30),
    )(query, offset, *accs, *sum(toks, []), *first[middle:], *second[middle:], *biases)
    key_cache, value_cache, bias = pl.pallas_call(
        store_kernel,
        out_shape=(cache, cache, bias_shape),
        in_specs=[VMEM] * 3,
        out_specs=(HBM,) * 3,
        scratch_shapes=[pltpu.SemaphoreType.DMA((3,))],
        name="store",
        **params(1),
    )(keys, values, bias)

    stages = exchanges(sp_count)
    for n, offsets in enumerate(stages):
        crossing = n < len(stages) // 2 * 2
        stats = [] if crossing else [stat]
        offsets = ((0,) if crossing else ()) + offsets
        for offset in offsets:
            perm = [
                (g * sp_count + i, (1 - g if crossing else g) * sp_count + (i ^ offset))
                for g in range(2)
                for i in range(sp_count)
            ]
            stats.append(lax.ppermute(stat, ("gr", "sp"), perm))
        offsets = offsets if crossing else (0,) + offsets
        stat = combine(stats, offsets, head_dim, n + 1 == len(stages))
    return key_cache, value_cache, jnp.transpose(bias, (0, 2, 1)), stat


def solution(mesh):
    in_specs = (
        P("gr", ("sp", "tp"), None),
        P("sp", None),
        P("sp", None),
        P("gr", None),
        P(),
        P("gr", ("sp", "tp"), None),
    )
    out_specs = (P("gr", "sp", "tp"), P("gr", "sp", "tp"), P("gr", "sp", "tp"), P("gr", "tp"))
    return jax.shard_map(
        per_device, mesh=mesh, in_specs=in_specs, out_specs=out_specs, check_vma=False
    )
```
